32 devices in a mesh: grp: 2 (over y), sp: 4 (over z), tp: 4 (over x, core).
Axes of the slice: x: 2, y: 2, z: 4, core: 2. Of those that a mesh axis runs over, the one named last changes fastest.
Arguments:
- gate_in: bfloat16 [4096, 1536], P(('grp', 'sp'), 'tp'), parts along dimension 0, may hold values from -6 to 6
- mult_in: bfloat16 [4096, 1536], P(('grp', 'sp'), 'tp'), parts along dimension 0, may hold values from -6 to 6
- value_in: bfloat16 [4096, 1536], P(('grp', 'sp'), 'tp'), parts along dimension 0, may hold values from -6 to 6
- doc_ids: int32 [4096], P(('grp', 'sp')), parts along dimension 0, may hold values from 0 to 1, never falling along the last dimension, each value on 1 to 1536 neighbouring positions
- conv_taps: bfloat16 [3, 1536], P(None, 'tp'), may hold values from -3 to 3
- out_proj: bfloat16 [1536, 2048], P('tp'), may hold values from -0.15625 to 0.15625
- resid: bfloat16 [4096, 2048], P(('grp', 'sp', 'tp')), parts along dimension 0, may hold values from -6 to 6
- norm1_gain: float32 [2048], replicated, may hold values from 0.1 to 1.9
- norm1_bias: float32 [2048], replicated, may hold values from -1.5 to 1.5
- expert_ids: int32 [4096, 2], P(('grp', 'sp', 'tp')), parts along dimension 0, may hold values from 0 to 3, all different within a row; in each aligned block of 128 rows (0 to 127, 128 to 255, ...) at most 80 rows name the same one
- expert_wts: float32 [4096, 2], P(('grp', 'sp', 'tp')), parts along dimension 0, may hold values from 0.1 to 1
- w_gate: bfloat16 [4, 2048, 3072], P('sp', None, 'tp'), may hold values from -0.125 to 0.125
- w_up: bfloat16 [4, 2048, 3072], P('sp', None, 'tp'), may hold values from -0.125 to 0.125
- w_down: bfloat16 [4, 3072, 2048], P('sp', 'tp'), may hold values from -0.21582031 to 0.21582031
- norm2_gain: float32 [2048], replicated, may hold values from 0.1 to 1.9
- norm2_bias: float32 [2048], replicated, may hold values from -1.5 to 1.5
Outputs:
- result: bfloat16 [4096, 2048], P(('grp', 'sp', 'tp')), parts along dimension 0
The draws below stay inside these ranges and needn't reach their ends.
There are 2 independent parts, one for each index of `grp`. The reference program is written for one: setup_inputs(seed, part) draws one part's arguments, and reference() takes and returns one part's arrays. A program takes and returns all parts, laid end to end along the dimension named above; an argument that names none is the same for every part. Nothing has to cross between parts.
Inputs may be any that keep to these rules, and one draw needn't show every extreme that they name: `doc_ids`: never falling along the sequence; each document has 1 to 1536 positions and one has exactly 1536. `expert_ids`: each row names 2 different experts. Among the rows of one device no expert is named more than 80 times, and in some device's rows some expert is named exactly 80 times.
All inputs are finite; a program needn't handle non-finite values.
Results may differ from the reference program's by a relative error of at most 0.0095.
Values may be sent and summed in bfloat16 or wider, within the bound.
A program may use at most 128 MiB of HBM per device.

```python
import math
import jax
import jax.numpy as jnp
import numpy as np
from jax import lax

D = 2048
D_CONV = 1536
FF_E = 3072
KW = 3
TOPK = 2
TOK_DEV = 128
TOKENS = 2048
EXPERTS = 4
CAP = 80
DOCS = 2
DOC_MOST = 1536
N_TP = 4


def block_levels(rng, extent, shards, smallest, largest):
    loudness, own = 1.0, jax.random.fold_in(rng, 6)
    for dim, shards_of in shards:
        steps = jnp.exp(jax.random.uniform(jax.random.fold_in(own, dim), (shards_of,), jnp.float32, smallest / len(shards), largest / len(shards)))
        loudness = loudness * jnp.repeat(steps, extent[dim] // shards_of).reshape([-1 if axis == dim else 1 for axis in range(len(extent))])
    return loudness


def profile(number_of, total, reach, skew):
    weights = [(1 << 20) // math.isqrt(grade ** skew) + 1 for grade in range(2, number_of + 1)]
    surplus, counts = total - reach - (number_of - 1), [1] * (number_of - 1)
    while surplus > 0:
        candidates = [i for i in range(number_of - 1) if counts[i] < reach]
        whole, left = sum([weights[i] for i in candidates]), surplus
        for i in candidates:
            extra = min(reach - counts[i], max(1, left * weights[i] // whole), surplus)
            counts[i] = counts[i] + extra
            surplus = surplus - extra
    return np.array([reach] + counts)


def ragged_sizes(rng, number_of, total, limit, lean):
    if number_of == 2:
        one = jax.random.randint(rng, (), max(1, total - limit), min(limit, total - 1) + 1)
        return jnp.stack([one, total - one])
    tallies = jnp.asarray(profile(number_of, total, limit, lean), jnp.int32)
    twos = (number_of - 1) // 2
    donor, receiver = tallies[1:1 + 2 * twos:2], tallies[2:2 + 2 * twos:2]
    room = jnp.minimum(donor - 1, limit - receiver)
    moved = jax.random.randint(jax.random.fold_in(rng, 1), (twos,), 0, 1 << 20) % (room + 1)
    tallies = tallies.at[1:1 + 2 * twos:2].set(donor - moved).at[2:2 + 2 * twos:2].set(receiver + moved)
    return tallies[jax.random.permutation(jax.random.fold_in(rng, 2), number_of)]


def routed_block(key, own, number, rows, number_of, top, most, lean):
    ranking = jax.random.permutation(key, number_of)
    packed, ordinary = shares(number_of, rows * top, most, lean, True), shares(number_of, rows * top, most, lean, False)
    places = jnp.arange(number_of)

    def named(lengths, offset_by):
        used = int((lengths > 0).sum())
        fixed = max(1, used // 4)
        passed = fixed + (places - fixed + offset_by * (used - fixed)) % max(1, number_of - fixed)
        return jnp.zeros((number_of,), jnp.int32).at[ranking[jnp.where(places < fixed, places, passed)]].set(jnp.asarray(lengths, jnp.int32))

    lengths = jnp.where(number % 4 == 0, named(packed, number // 4), named(ordinary, number - number // 4 - 1))
    mixed = jax.random.permutation(jax.random.fold_in(own, 3), number_of)
    donor, receiver = mixed[0:number_of // 2 * 2:2], mixed[1:number_of // 2 * 2:2]
    slack = jnp.minimum(lengths[donor] - 1, most - lengths[receiver]) // 2
    slack = jnp.where((donor == ranking[0]) | (receiver == ranking[0]) | (lengths[receiver] == 0), 0, jnp.maximum(slack, 0))
    passed = jax.random.randint(jax.random.fold_in(own, 4), (number_of // 2,), 0, 1 << 20) % (slack + 1)
    lengths = lengths.at[donor].add(-passed).at[receiver].add(passed)
    items = jnp.searchsorted(jnp.cumsum(lengths), jnp.arange(rows * top), side="right").astype(jnp.int32)
    table = items.reshape(top, rows).T
    table = table[jax.random.permutation(jax.random.fold_in(own, 1), rows)]
    offset_by = jax.random.randint(jax.random.fold_in(own, 2), (rows, 1), 0, top)
    return jnp.take_along_axis(table, (jnp.arange(top)[None, :] + offset_by) % top, axis=1)


def shares(number_of, total, limit, skew, full):
    portions = [(1 << 20) // math.isqrt(grade ** skew) + 1 for grade in range(1, number_of + 1)]
    largest = limit if full else min(limit, max(-(-total // number_of), total * portions[0] // sum(portions)))
    least = 1 if total - largest >= number_of - 1 else 0
    counts, surplus = [largest] + [least] * (number_of - 1), total - largest - least * (number_of - 1)
    while surplus > 0:
        candidates = [i for i in range(1, number_of) if counts[i] < largest] or [i for i in range(1, number_of) if counts[i] < limit]
        whole, left = sum([portions[i] for i in candidates]), surplus
        for i in candidates:
            more = min(limit - counts[i], max(1, left * portions[i] // whole), surplus)
            counts[i] = counts[i] + more
            surplus = surplus - more
    return np.array(counts)


def scatter_about(own_key, extent, width, most, split=(), kind=jnp.bfloat16):
    result = jax.random.normal(own_key, extent, jnp.float32) * width
    if len(split) > 0:
        result = block_levels(own_key, extent, split, -0.22, 0.18) * result
    return jnp.clip(result, min=-most, max=most).astype(kind)


def setup_inputs(seed: int = 0, part: int = 0) -> dict:
    streams_of = jax.random.split(jax.random.key(seed), 17)
    part_keys = jax.random.split(jax.random.fold_in(streams_of[16], part), 17)
    gate_in = scatter_about(part_keys[0], (TOKENS, D_CONV), 1.0, 6.0, ((0, 4), (1, 4)))
    mult_in = scatter_about(part_keys[1], (TOKENS, D_CONV), 1.0, 6.0, ((0, 4), (1, 4)))
    value_in = scatter_about(part_keys[2], (TOKENS, D_CONV), 1.0, 6.0, ((0, 4), (1, 4)))
    doc_ids = jnp.searchsorted(jnp.cumsum(ragged_sizes(part_keys[3], DOCS, TOKENS, DOC_MOST, 1)), jnp.arange(TOKENS), side="right").astype(jnp.int32)
    conv_taps = scatter_about(streams_of[4], (KW, D_CONV), 0.577, 3.0, ((1, 4),))
    out_proj = scatter_about(streams_of[5], (D_CONV, D), D_CONV ** -0.5, 0.15625, ((0, 4),))
    resid = scatter_about(part_keys[6], (TOKENS, D), 1.0, 6.0, ((0, 16),))
    norm1_gain = jnp.clip(1.0 + 0.18 * jax.random.normal(streams_of[7], (D,), jnp.float32), 0.1, 1.9)
    norm1_bias = scatter_about(streams_of[8], (D,), 0.3, 1.5, (), jnp.float32)
    expert_ids_keys = jax.random.split(jax.random.fold_in(part_keys[9], 1), TOKENS // TOK_DEV)
    expert_ids_turns = jax.random.permutation(jax.random.fold_in(part_keys[9], 3), TOKENS // TOK_DEV)
    expert_ids = jax.vmap(lambda own, number: routed_block(jax.random.fold_in(part_keys[9], 2), own, number, TOK_DEV, EXPERTS, TOPK, CAP, 2))(expert_ids_keys, expert_ids_turns).reshape((TOKENS, TOPK))
    expert_wts = jnp.clip(0.1 + 0.9 * jax.random.uniform(part_keys[10], (TOKENS, TOPK), jnp.float32) ** block_levels(part_keys[10], (TOKENS, TOPK), ((0, 16),), -0.2, 0.2), 0.1, 1.0)
    w_gate = scatter_about(streams_of[11], (EXPERTS, D, FF_E), D ** -0.5, 0.125, ((0, 4), (2, 4)))
    w_up = scatter_about(streams_of[12], (EXPERTS, D, FF_E), D ** -0.5, 0.125, ((0, 4), (2, 4)))
    w_down = scatter_about(streams_of[13], (EXPERTS, FF_E, D), (2.0 / FF_E ** 0.5), 0.21582031, ((0, 4), (1, 4)))
    norm2_gain = jnp.clip(1.0 + 0.18 * jax.random.normal(streams_of[14], (D,), jnp.float32), 0.1, 1.9)
    norm2_bias = scatter_about(streams_of[15], (D,), 0.3, 1.5, (), jnp.float32)
    return dict(gate_in=gate_in, mult_in=mult_in, value_in=value_in, doc_ids=doc_ids, conv_taps=conv_taps, out_proj=out_proj, resid=resid, norm1_gain=norm1_gain, norm1_bias=norm1_bias, expert_ids=expert_ids, expert_wts=expert_wts, w_gate=w_gate, w_up=w_up, w_down=w_down, norm2_gain=norm2_gain, norm2_bias=norm2_bias)


residual_scale = 2.0 ** 0.5
norm_eps = 1e-05

def layer_norm(pre, gain, bias):
    center = pre - lax.optimization_barrier(jnp.mean(pre, axis=-1, keepdims=True))
    spread = lax.optimization_barrier(jnp.mean(center * center, axis=-1, keepdims=True))
    return center * lax.rsqrt(spread + norm_eps) * gain + bias

def reference(gate_in, mult_in, value_in, doc_ids, conv_taps, out_proj, resid, norm1_gain, norm1_bias, expert_ids, expert_wts, w_gate, w_up, w_down, norm2_gain, norm2_bias):
    tap_weights = conv_taps.astype(jnp.float32)
    product = mult_in.astype(jnp.float32) * value_in.astype(jnp.float32)
    row_count = product.shape[0]
    padded = jnp.pad(product, ((KW - 1, 0), (0, 0)))
    doc_padded = jnp.concatenate([jnp.full((KW - 1,), -1, jnp.int32), doc_ids.astype(jnp.int32)])
    filtered = jnp.zeros_like(product)
    for tap_index in range(KW):
        shifted = padded[tap_index:tap_index + row_count]
        same_doc = (doc_padded[tap_index:tap_index + row_count] == doc_ids)[:, None]
        filtered = filtered + tap_weights[tap_index] * jnp.where(same_doc, shifted, 0.0)
    mixed_heads = (gate_in.astype(jnp.float32) * filtered).astype(jnp.bfloat16)
    mixed = jnp.dot(mixed_heads, out_proj, preferred_element_type=jnp.float32)
    hidden_one = layer_norm(residual_scale * resid.astype(jnp.float32) + mixed, norm1_gain, norm1_bias).astype(jnp.bfloat16)
    flat_ids = expert_ids.reshape(-1)
    flat_wts = expert_wts.reshape(-1)
    most_rows = CAP * (TOKENS // TOK_DEV)
    part_width = FF_E // N_TP

    def one_expert(moe, inputs):
        gate_w, up_w, down_w, number = inputs
        chosen = flat_ids == number
        picks = jnp.nonzero(chosen, size=most_rows, fill_value=0)[0].astype(jnp.int32)
        live = jnp.arange(most_rows, dtype=jnp.int32) < jnp.sum(chosen.astype(jnp.int32))
        rows = (picks // TOPK).astype(jnp.int32)
        inputs_rows = hidden_one[rows]
        gate_act = jnp.dot(inputs_rows, gate_w, preferred_element_type=jnp.float32)
        up_act = jnp.dot(inputs_rows, up_w, preferred_element_type=jnp.float32)
        hid = (jax.nn.silu(gate_act) * up_act).astype(jnp.bfloat16)
        total = jnp.zeros((most_rows, D), jnp.float32)
        for part in range(N_TP):
            piece = jnp.dot(hid[:, part * part_width:(part + 1) * part_width], down_w[part * part_width:(part + 1) * part_width], preferred_element_type=jnp.float32).astype(jnp.bfloat16)
            total = total + lax.optimization_barrier(piece).astype(jnp.float32)
        expert_out = lax.optimization_barrier(total.astype(jnp.bfloat16)).astype(jnp.float32)
        weight = jnp.where(live, flat_wts[picks], 0.0)
        return (moe.at[rows].add(weight[:, None] * expert_out), None)
    moe_start = jnp.zeros((row_count, D), jnp.float32)
    numbers = jnp.arange(EXPERTS, dtype=jnp.int32)
    moe, _ = lax.scan(one_expert, moe_start, (w_gate, w_up, w_down, numbers))
    return layer_norm(residual_scale * hidden_one.astype(jnp.float32) + moe, norm2_gain, norm2_bias).astype(jnp.bfloat16)
```

```python
import functools

import jax
import jax.numpy as jnp
from jax import lax
from jax.experimental import pallas as pl
from jax.experimental.pallas import tpu as pltpu
from jax.sharding import PartitionSpec as P

residual_scale = 2.0**0.5
norm_eps = 1e-05
MESH = pl.DeviceIdType.MESH
f32, bf16 = jnp.float32, jnp.bfloat16


def layer_norm(pre, gain, bias):
    center = pre - jnp.mean(pre, axis=-1, keepdims=True)
    spread = jnp.mean(center * center, axis=-1, keepdims=True)
    return center * lax.rsqrt(spread + norm_eps) * gain + bias


def remote(src, dst, send, recv, **where):
    return pltpu.make_async_remote_copy(
        src_ref=src, dst_ref=dst, send_sem=send, recv_sem=recv, device_id=where, device_id_type=MESH
    )


def kernel(
    experts, slots,
    gate_h, mult_h, value_h, docs_h, taps, proj_h, resid_h, gain1, bias1, ids, wts,
    w_gate_h, w_up_h, w_down_h, gain2, bias2,
    out,
    gate, mult, value, docs, proj, resid, w_gate, w_up, w_down,
    edge_m, edge_v, edge_d, ext, ext_docs, heads,
    send1, got1, send2, got2, own, hidden, slot_of, weight_of,
    packed, rows, part, hid, sum_in, sum_send, cross_in, done_out, back, moe,
    local, edge_s, edge_r, mix_s, mix_r,
    zs, zr, xs, xr, bs, br, cs, cr, r1s, r1r, r2s, r2r, r3s, r3r,
):
    s, t = lax.axis_index("sp"), lax.axis_index("tp")
    hi, lo = t // 2, t % 2
    sib, far = hi * 2 + (1 - lo), (1 - hi) * 2 + lo
    count, model = resid.shape
    length, channels = mult.shape
    taps_n = taps.shape[0]
    top = ids.shape[0]

    loads = [
        pltpu.make_async_copy(a, b, local.at[i])
        for i, (a, b) in enumerate(
            [(mult_h, mult), (value_h, value), (docs_h, docs), (gate_h, gate), (proj_h, proj),
             (resid_h, resid), (w_gate_h, w_gate), (w_up_h, w_up), (w_down_h, w_down)]
        )
    ]
    for c in loads:
        c.start()

    barrier = pltpu.get_barrier_semaphore()

    def greet(d, _):
        pl.semaphore_signal(barrier, inc=1, device_id={"sp": (s + d) % experts}, device_id_type=MESH)
        return 0

    lax.fori_loop(1, experts, greet, 0)
    pl.semaphore_signal(barrier, inc=1, device_id={"tp": sib}, device_id_type=MESH)
    pl.semaphore_signal(barrier, inc=1, device_id={"tp": far}, device_id_type=MESH)
    pl.semaphore_wait(barrier, experts + 1)

    nxt = (s + 1) % experts
    edges = [
        remote(mult_h.at[pl.ds(length - 16, 16)], edge_m, edge_s.at[0], edge_r.at[0], sp=nxt),
        remote(value_h.at[pl.ds(length - 16, 16)], edge_v, edge_s.at[1], edge_r.at[1], sp=nxt),
        remote(docs_h.at[pl.ds(length - 8, 8)], edge_d, edge_s.at[2], edge_r.at[2], sp=nxt),
    ]
    for c in edges:
        c.start()

    padded = slot_of.shape[0]
    expert_no = lax.broadcasted_iota(jnp.int32, (padded, count), 0)
    chosen = jnp.zeros((padded, count), f32)
    weight = jnp.zeros((padded, count), f32)
    for k in range(top):
        same = ids[k : k + 1, :] == expert_no
        chosen = chosen + jnp.where(same, 1.0, 0.0)
        weight = weight + jnp.where(same, wts[k : k + 1, :], 0.0)
    before = lax.broadcasted_iota(jnp.int32, (count, count), 0) < lax.broadcasted_iota(
        jnp.int32, (count, count), 1
    )
    rank = jnp.dot(chosen.astype(bf16), jnp.where(before, 1.0, 0.0).astype(bf16), preferred_element_type=f32)
    slot_of[...] = jnp.where(chosen > 0.5, rank, -1.0)
    weight_of[...] = weight

    for c in loads[:4]:
        c.wait()
    for r in range(0, length, 128):
        ext[8 + r : 8 + r + 128, :] = mult[r : r + 128, :].astype(f32) * value[r : r + 128, :].astype(f32)
    ext_docs[8:, :] = docs[...]
    for c in edges:
        c.wait_recv()
    ext[0:8, :] = (edge_m[...].astype(f32) * edge_v[...].astype(f32))[8:16, :]
    ext_docs[0:8, :] = jnp.where(s > 0, edge_d[...], -1)
    for r in range(0, length, 64):
        now = ext_docs[8 + r : 8 + r + 64, :]
        same = [ext_docs[8 + r - b : 8 + r - b + 64, :] == now for b in range(1, taps_n)]
        for c in range(0, channels, 128):
            acc = taps[taps_n - 1 :, c : c + 128] * ext[8 + r : 8 + r + 64, c : c + 128]
            for b in range(1, taps_n):
                moved = ext[8 + r - b : 8 + r - b + 64, c : c + 128]
                acc = acc + taps[taps_n - 1 - b : taps_n - b, c : c + 128] * jnp.where(same[b - 1], moved, 0.0)
            heads[r : r + 64, c : c + 128] = (gate[r : r + 64, c : c + 128].astype(f32) * acc).astype(bf16)

    loads[4].wait()
    wide = 512

    def projected(number, n):
        return jnp.dot(
            heads[pl.ds(pl.multiple_of(number * count, count), count), :], proj[:, n : n + wide],
            preferred_element_type=f32,
        )

    mix = []
    for i, h in enumerate((1 - hi, hi)):
        for n in range(0, model, wide):
            send1[i, :, n : n + wide] = projected(h * 2 + (1 - lo), n).astype(bf16)
        c = remote(send1.at[i], got1.at[i], mix_s.at[i], mix_r.at[i], tp=sib)
        c.start()
        mix.append(c)
    for n in range(0, model, wide):
        own[:, n : n + wide] = projected((1 - hi) * 2 + lo, n)
    mix[0].wait_recv()
    for n in range(0, model, wide):
        send2[:, n : n + wide] = (own[:, n : n + wide] + got1[0, :, n : n + wide].astype(f32)).astype(bf16)
    c = remote(send2, got2, mix_s.at[2], mix_r.at[2], tp=far)
    c.start()
    mix.append(c)
    for n in range(0, model, wide):
        own[:, n : n + wide] = projected(t, n)
    loads[5].wait()
    mix[1].wait_recv()
    for n in range(0, model, wide):
        q = slice(n, n + wide)
        own[:, q] = own[:, q] + got1[1, :, q].astype(f32) + residual_scale * resid[:, q].astype(f32)
    mix[2].wait_recv()
    for r in range(0, count, 32):
        q = slice(r, r + 32)
        hidden[q, :] = layer_norm(own[q, :] + got2[q, :].astype(f32), gain1[...], bias1[...]).astype(bf16)

    slot_no = lax.broadcasted_iota(jnp.int32, (slots, count), 0).astype(f32)

    def selected(e):
        return slot_no == slot_of[pl.ds(e, 1), :]

    def pack(e):
        pick = jnp.where(selected(e), 1.0, 0.0).astype(bf16)
        return jnp.dot(pick, hidden[...], preferred_element_type=f32).astype(bf16)

    def home(d):
        return (s - d + experts) % experts

    def z_out(d):
        return remote(packed.at[d], rows.at[s, lo, hi], zs.at[d], zr.at[d], sp=(s + d) % experts)

    def x_copy(d):
        block = rows.at[home(d), lo, hi]
        return remote(block, block, xs.at[d], xr.at[d], tp=far)

    def b_copy(d):
        block = rows.at[home(d), lo, hi]
        return remote(block, block, bs.at[d], br.at[d], tp=sib)

    def c_copy(d):
        block = rows.at[home(d), lo, 1 - hi]
        return remote(block, block, cs.at[d], cr.at[d], tp=sib)

    def r1_copy(d):
        return remote(part.at[home(d), 1 - lo], sum_in.at[home(d)], r1s.at[d], r1r.at[d], tp=sib)

    def r2_copy(d):
        return remote(sum_send.at[d], cross_in.at[d], r2s.at[d], r2r.at[d], tp=far)

    def r3_copy(d):
        return remote(done_out.at[d], back.at[s], r3s.at[d], r3r.at[d], sp=home(d))

    rows[s, lo, hi] = pack(s)
    x_copy(0).start()
    b_copy(0).start()

    def dispatch(d, _):
        packed[d] = pack((s + d) % experts)
        z_out(d).start()
        return 0

    lax.fori_loop(1, experts, dispatch, 0)

    for c in loads[6:]:
        c.wait()

    def experts_of(j):
        size = 4 * slots
        step = 256
        for n in range(0, w_gate.shape[1], step):
            x = rows[j].reshape(size, model)
            g = jnp.dot(x, w_gate[:, n : n + step], preferred_element_type=f32)
            u = jnp.dot(x, w_up[:, n : n + step], preferred_element_type=f32)
            hid[:, n : n + step] = (jax.nn.silu(g) * u).astype(bf16)
        for n in range(0, model, step):
            y = jnp.dot(hid[...], w_down[:, n : n + step], preferred_element_type=f32)
            part[j, :, :, :, n : n + step] = y.astype(bf16).reshape(2, 2, slots, step)

    def turn(d, _):
        @pl.when(jnp.logical_and(d > 0, d < experts))
        def _():
            z_out(d).wait_recv()
            x_copy(d).start()
            b_copy(d).start()

        @pl.when(d >= 3)
        def _():
            b = d - 3
            r2_copy(b).wait_recv()
            j = home(b)
            total = part[j, lo, hi].astype(f32) + sum_in[j, hi].astype(f32) + cross_in[b].astype(f32)
            done_out[b] = total.astype(bf16)

            @pl.when(b > 0)
            def _():
                r3_copy(b).start()

        @pl.when(jnp.logical_and(d >= 2, d < experts + 2))
        def _():
            b = d - 2
            r1_copy(b).wait_recv()
            j = home(b)
            sum_send[b] = (part[j, lo, 1 - hi].astype(f32) + sum_in[j, 1 - hi].astype(f32)).astype(bf16)
            r2_copy(b).start()

        @pl.when(jnp.logical_and(d >= 1, d < experts + 1))
        def _():
            b = d - 1
            x_copy(b).wait_recv()
            c_copy(b).start()
            b_copy(b).wait_recv()
            c_copy(b).wait_recv()
            experts_of(home(b))
            r1_copy(b).start()

        return 0

    lax.fori_loop(0, experts + 3, turn, 0)

    def weighted(e, value_of):
        pick = jnp.where(selected(e), weight_of[pl.ds(e, 1), :], 0.0)
        high = pick.astype(bf16)
        low = (pick - high.astype(f32)).astype(bf16)
        dims = (((0,), (0,)), ((), ()))
        return lax.dot_general(high, value_of, dims, preferred_element_type=f32) + lax.dot_general(
            low, value_of, dims, preferred_element_type=f32
        )

    moe[...] = residual_scale * hidden[...].astype(f32) + weighted(s, done_out[0])

    def combine(d, _):
        r3_copy(d).wait_recv()
        e = (s + d) % experts
        moe[...] += weighted(e, back[e])
        return 0

    lax.fori_loop(1, experts, combine, 0)
    for r in range(0, count, 32):
        q = slice(r, r + 32)
        out[q, :] = layer_norm(moe[q, :], gain2[...], bias2[...]).astype(bf16)

    for c in edges + mix:
        c.wait_send()

    def drain(d, _):
        for c in (x_copy, b_copy, c_copy, r1_copy, r2_copy):
            c(d).wait_send()

        @pl.when(d > 0)
        def _():
            z_out(d).wait_send()
            r3_copy(d).wait_send()

        return 0

    lax.fori_loop(0, experts, drain, 0)


def shards(
    gate_in, mult_in, value_in, doc_ids, conv_taps, out_proj, resid, norm1_gain, norm1_bias,
    expert_ids, expert_wts, w_gate, w_up, w_down, norm2_gain, norm2_bias,
):
    experts, parts = lax.axis_size("sp"), lax.axis_size("tp")
    assert parts == 4
    length, channels = mult_in.shape
    count, model = resid.shape
    top = expert_ids.shape[1]
    units = w_gate.shape[2]
    capacity = 5 * count * top // (4 * experts)
    slots = -(-capacity // 16) * 16
    padded = max(8, experts)
    docs = jnp.broadcast_to(doc_ids[:, None], (length, 128))
    vmem = pl.BlockSpec(memory_space=pltpu.VMEM)
    hbm = pl.BlockSpec(memory_space=pl.ANY)
    V = pltpu.VMEM
    sems = pltpu.SemaphoreType.DMA
    blocks = (experts, slots, model)
    return pl.pallas_call(
        functools.partial(kernel, experts, slots),
        out_shape=jax.ShapeDtypeStruct((count, model), bf16),
        in_specs=[hbm, hbm, hbm, hbm, vmem, hbm, hbm, vmem, vmem, vmem, vmem, hbm, hbm, hbm, vmem, vmem],
        out_specs=vmem,
        scratch_shapes=[
            V((length, channels), bf16), V((length, channels), bf16), V((length, channels), bf16),
            V((length, 128), jnp.int32), V((channels, model), bf16), V((count, model), bf16),
            V((model, units), bf16), V((model, units), bf16), V((units, model), bf16),
            V((16, channels), bf16), V((16, channels), bf16), V((8, 128), jnp.int32),
            V((length + 8, channels), f32), V((length + 8, 128), jnp.int32), V((length, channels), bf16),
            V((2, count, model), bf16), V((2, count, model), bf16), V((count, model), bf16),
            V((count, model), bf16), V((count, model), f32), V((count, model), bf16),
            V((padded, count), f32), V((padded, count), f32),
            V(blocks, bf16), V((experts, 2, 2, slots, model), bf16), V((experts, 2, 2, slots, model), bf16),
            V((4 * slots, units), bf16), V((experts, 2, slots, model), bf16), V(blocks, bf16),
            V(blocks, bf16), V(blocks, bf16), V(blocks, bf16), V((count, model), f32),
            sems((9,)), sems((3,)), sems((3,)), sems((3,)), sems((3,)),
        ] + [sems((experts,))] * 14,
        compiler_params=pltpu.CompilerParams(
            collective_id=0, has_side_effects=True, vmem_limit_bytes=62 * 2**20
        ),
    )(
        gate_in, mult_in, value_in, docs, conv_taps.astype(f32), out_proj, resid,
        norm1_gain[None], norm1_bias[None], expert_ids.T, expert_wts.T,
        w_gate[0], w_up[0], w_down[0], norm2_gain[None], norm2_bias[None],
    )


def solution(mesh):
    placed = (
        P(("grp", "sp"), "tp"),
        P(("grp", "sp"), "tp"),
        P(("grp", "sp"), "tp"),
        P(("grp", "sp")),
        P(None, "tp"),
        P("tp", None),
        P(("grp", "sp", "tp"), None),
        P(),
        P(),
        P(("grp", "sp", "tp"), None),
        P(("grp", "sp", "tp"), None),
        P("sp", None, "tp"),
        P("sp", None, "tp"),
        P("sp", "tp", None),
        P(),
        P(),
    )
    return jax.shard_map(
        shards, mesh=mesh, in_specs=placed, out_specs=P(("grp", "sp", "tp"), None), check_vma=False
    )
```

```python
import functools

import jax
import jax.numpy as jnp
from jax import lax
from jax.experimental import pallas as pl
from jax.experimental.pallas import tpu as pltpu
from jax.sharding import PartitionSpec as P

residual_scale = 2.0**0.5
norm_eps = 1e-05
MESH = pl.DeviceIdType.MESH
f32, bf16 = jnp.float32, jnp.bfloat16


def layer_norm(pre, gain, bias):
    center = pre - jnp.mean(pre, axis=-1, keepdims=True)
    spread = jnp.mean(center * center, axis=-1, keepdims=True)
    return center * lax.rsqrt(spread + norm_eps) * gain + bias


def remote(src, dst, send, recv, **where):
    return pltpu.make_async_remote_copy(
        src_ref=src, dst_ref=dst, send_sem=send, recv_sem=recv, device_id=where, device_id_type=MESH
    )


def kernel(
    experts, slots, piece,
    gate_h, mult_h, value_h, docs_h, taps, proj_h, resid_h, gain1, bias1, ids, wts,
    w_gate_h, w_up_h, w_down_h, gain2, bias2,
    out,
    gate, mult, value, docs, proj, resid, w_gate, w_up, w_down,
    edge_m, edge_v, edge_d, ext, ext_docs, heads,
    send1, got1, send2, got2, own, hidden, slot_of, weight_of,
    packed, rows, part, hid, sum_in, sum_send, cross_in, done_out, back, picks,
    local, edge_s, edge_r, mix_s, mix_r,
    zs, zr, xs, xr, bs, br, cs, cr, r1s, r1r, r2s, r2r, r3s, r3r,
):
    s, t = lax.axis_index("sp"), lax.axis_index("tp")
    hi, lo = t // 2, t % 2
    sib, far = hi * 2 + (1 - lo), (1 - hi) * 2 + lo
    count, model = resid.shape
    length, channels = mult.shape
    taps_n = taps.shape[0]
    top = ids.shape[0]

    loads = [
        pltpu.make_async_copy(a, b, local.at[i])
        for i, (a, b) in enumerate(
            [(mult_h, mult), (value_h, value), (docs_h, docs), (gate_h, gate), (proj_h, proj),
             (resid_h, resid), (w_gate_h, w_gate), (w_up_h, w_up), (w_down_h, w_down)]
        )
    ]
    for c in loads:
        c.start()

    barrier = pltpu.get_barrier_semaphore()

    def greet(d, _):
        pl.semaphore_signal(barrier, inc=1, device_id={"sp": (s + d) % experts}, device_id_type=MESH)
        return 0

    lax.fori_loop(1, experts, greet, 0)
    pl.semaphore_signal(barrier, inc=1, device_id={"tp": sib}, device_id_type=MESH)
    pl.semaphore_signal(barrier, inc=1, device_id={"tp": far}, device_id_type=MESH)
    pl.semaphore_wait(barrier, experts + 1)

    nxt = (s + 1) % experts
    edges = [
        remote(mult_h.at[pl.ds(length - 16, 16)], edge_m, edge_s.at[0], edge_r.at[0], sp=nxt),
        remote(value_h.at[pl.ds(length - 16, 16)], edge_v, edge_s.at[1], edge_r.at[1], sp=nxt),
        remote(docs_h.at[pl.ds(length - 8, 8)], edge_d, edge_s.at[2], edge_r.at[2], sp=nxt),
    ]
    for c in edges:
        c.start()

    padded = slot_of.shape[0]
    expert_no = lax.broadcasted_iota(jnp.int32, (padded, count), 0)
    chosen = jnp.zeros((padded, count), f32)
    weight = jnp.zeros((padded, count), f32)
    for k in range(top):
        same = ids[k : k + 1, :] == expert_no
        chosen = chosen + jnp.where(same, 1.0, 0.0)
        weight = weight + jnp.where(same, wts[k : k + 1, :], 0.0)
    before = lax.broadcasted_iota(jnp.int32, (count, count), 0) < lax.broadcasted_iota(
        jnp.int32, (count, count), 1
    )
    rank = jnp.dot(chosen.astype(bf16), jnp.where(before, 1.0, 0.0).astype(bf16), preferred_element_type=f32)
    slot_of[...] = jnp.where(chosen > 0.5, rank, -1.0)
    weight_of[...] = weight

    for c in loads[:4]:
        c.wait()
    for r in range(0, length, 128):
        ext[8 + r : 8 + r + 128, :] = mult[r : r + 128, :].astype(f32) * value[r : r + 128, :].astype(f32)
    ext_docs[8:, :] = docs[...]
    for c in edges:
        c.wait_recv()
    ext[0:8, :] = (edge_m[...].astype(f32) * edge_v[...].astype(f32))[8:16, :]
    ext_docs[0:8, :] = jnp.where(s > 0, edge_d[...], -1)
    for r in range(0, length, 64):
        now = ext_docs[8 + r : 8 + r + 64, :]
        same = [ext_docs[8 + r - b : 8 + r - b + 64, :] == now for b in range(1, taps_n)]
        for c in range(0, channels, 128):
            acc = taps[taps_n - 1 :, c : c + 128] * ext[8 + r : 8 + r + 64, c : c + 128]
            for b in range(1, taps_n):
                moved = ext[8 + r - b : 8 + r - b + 64, c : c + 128]
                acc = acc + taps[taps_n - 1 - b : taps_n - b, c : c + 128] * jnp.where(same[b - 1], moved, 0.0)
            heads[r : r + 64, c : c + 128] = (gate[r : r + 64, c : c + 128].astype(f32) * acc).astype(bf16)

    loads[4].wait()
    wide = 512

    def projected(number, n):
        return jnp.dot(
            heads[pl.ds(pl.multiple_of(number * count, count), count), :], proj[:, n : n + wide],
            preferred_element_type=f32,
        )

    mix = []
    for i, h in enumerate((1 - hi, hi)):
        for n in range(0, model, wide):
            send1[i, :, n : n + wide] = projected(h * 2 + (1 - lo), n).astype(bf16)
        c = remote(send1.at[i], got1.at[i], mix_s.at[i], mix_r.at[i], tp=sib)
        c.start()
        mix.append(c)
    for n in range(0, model, wide):
        own[:, n : n + wide] = projected((1 - hi) * 2 + lo, n)
    mix[0].wait_recv()
    for n in range(0, model, wide):
        send2[:, n : n + wide] = (own[:, n : n + wide] + got1[0, :, n : n + wide].astype(f32)).astype(bf16)
    c = remote(send2, got2, mix_s.at[2], mix_r.at[2], tp=far)
    c.start()
    mix.append(c)
    for n in range(0, model, wide):
        own[:, n : n + wide] = projected(t, n)
    loads[5].wait()
    mix[1].wait_recv()
    for n in range(0, model, wide):
        q = slice(n, n + wide)
        own[:, q] = own[:, q] + got1[1, :, q].astype(f32) + residual_scale * resid[:, q].astype(f32)
    mix[2].wait_recv()
    for r in range(0, count, 32):
        q = slice(r, r + 32)
        hidden[q, :] = layer_norm(own[q, :] + got2[q, :].astype(f32), gain1[...], bias1[...]).astype(bf16)

    slot_no = lax.broadcasted_iota(jnp.int32, (slots, count), 0).astype(f32)
    mine, other = lo * 2 + hi, lo * 2 + 1 - hi
    pieces = slots // piece

    def selected(e):
        return slot_no == slot_of[pl.ds(e, 1), :]

    def pack(e):
        pick = jnp.where(selected(e), 1.0, 0.0).astype(bf16)
        return jnp.dot(pick, hidden[...], preferred_element_type=f32).astype(bf16)

    def z_out(k, d):
        return remote(packed.at[k, d], rows.at[k, mine, s], zs.at[k, d], zr.at[k, d], sp=(s + d) % experts)

    def x_copy(k):
        block = rows.at[k, mine]
        return remote(block, block, xs.at[k], xr.at[k], tp=far)

    def b_copy(k):
        block = rows.at[k, mine]
        return remote(block, block, bs.at[k], br.at[k], tp=sib)

    def c_copy(k):
        block = rows.at[k, other]
        return remote(block, block, cs.at[k], cr.at[k], tp=sib)

    def r1_copy(k):
        return remote(part.at[k, pl.ds((1 - lo) * 2, 2)], sum_in.at[k], r1s.at[k], r1r.at[k], tp=sib)

    def r2_copy(k):
        return remote(sum_send.at[k], cross_in.at[k], r2s.at[k], r2r.at[k], tp=far)

    def r3_copy(k, d):
        to = (s - d + experts) % experts
        return remote(done_out.at[k, to], back.at[k, s], r3s.at[k, d], r3r.at[k, d], sp=to)

    def each(count_of, run):
        def step(i, _):
            run(i)
            return 0

        lax.fori_loop(0, count_of, step, 0)

    def across(run):
        def step(d, _):
            run(d)
            return 0

        lax.fori_loop(1, experts, step, 0)

    def pack_for(d):
        y = pack((s + d) % experts)
        for k in range(pieces):
            packed[k, d] = y[k * piece : (k + 1) * piece, :]

    across(pack_for)
    each(pieces, lambda k: across(lambda d: z_out(k, d).start()))
    y = pack(s)
    for k in range(pieces):
        rows[k, mine, s] = y[k * piece : (k + 1) * piece, :]

    def pick_for(e):
        pick = jnp.where(selected(e), weight_of[pl.ds(e, 1), :], 0.0)
        high = pick.astype(bf16)
        low = (pick - high.astype(f32)).astype(bf16)
        for k in range(pieces):
            picks[0, k, e] = high[k * piece : (k + 1) * piece, :]
            picks[1, k, e] = low[k * piece : (k + 1) * piece, :]

    each(experts, pick_for)
    for c in loads[6:]:
        c.wait()

    whole = 4 * experts * piece
    group = 4 if whole <= 512 else 1
    size = group * experts * piece

    def experts_of(k):
        def step(m, _):
            block = pl.ds(m * group, group)
            wide_f = 256
            for n in range(0, w_gate.shape[1], wide_f):
                x = rows[k, block].reshape(size, model)
                g = jnp.dot(x, w_gate[:, n : n + wide_f], preferred_element_type=f32)
                u = jnp.dot(x, w_up[:, n : n + wide_f], preferred_element_type=f32)
                hid[:, n : n + wide_f] = (jax.nn.silu(g) * u).astype(bf16)
            for n in range(0, model, wide_f):
                y = jnp.dot(hid[...], w_down[:, n : n + wide_f], preferred_element_type=f32)
                part[k, block, :, :, n : n + wide_f] = y.astype(bf16).reshape(group, experts, piece, wide_f)
            return 0

        lax.fori_loop(0, 4 // group, step, 0)

    def turn(d, _):
        @pl.when(d < pieces)
        def _():
            across(lambda i: z_out(d, i).wait_recv())
            x_copy(d).start()
            b_copy(d).start()

        @pl.when(d >= 3)
        def _():
            k = d - 3
            r2_copy(k).wait_recv()

            def add(j):
                total = part[k, mine, j].astype(f32) + sum_in[k, hi, j].astype(f32) + cross_in[k, j].astype(f32)
                done_out[k, j] = total.astype(bf16)

            each(experts, add)
            across(lambda i: r3_copy(k, i).start())
            back[k, s] = done_out[k, s]

        @pl.when(jnp.logical_and(d >= 2, d < pieces + 2))
        def _():
            k = d - 2
            r1_copy(k).wait_recv()

            def add(j):
                total = part[k, other, j].astype(f32) + sum_in[k, 1 - hi, j].astype(f32)
                sum_send[k, j] = total.astype(bf16)

            each(experts, add)
            r2_copy(k).start()

        @pl.when(jnp.logical_and(d >= 1, d < pieces + 1))
        def _():
            k = d - 1
            x_copy(k).wait_recv()
            c_copy(k).start()
            b_copy(k).wait_recv()
            c_copy(k).wait_recv()
            experts_of(k)
            r1_copy(k).start()

        return 0

    lax.fori_loop(0, pieces + 3, turn, 0)

    each(pieces, lambda k: across(lambda d: r3_copy(k, d).wait_recv()))
    dims = (((0,), (0,)), ((), ()))
    total_slots = pieces * experts * piece
    high = picks[0].reshape(total_slots, count)
    low = picks[1].reshape(total_slots, count)
    for n in range(0, model, 512):
        value_of = back[:, :, :, n : n + 512].reshape(total_slots, 512)
        own[:, n : n + 512] = (
            residual_scale * hidden[:, n : n + 512].astype(f32)
            + lax.dot_general(high, value_of, dims, preferred_element_type=f32)
            + lax.dot_general(low, value_of, dims, preferred_element_type=f32)
        )
    for r in range(0, count, 32):
        q = slice(r, r + 32)
        out[q, :] = layer_norm(own[q, :], gain2[...], bias2[...]).astype(bf16)

    for c in edges + mix:
        c.wait_send()

    def drain(k):
        for c in (x_copy, b_copy, c_copy, r1_copy, r2_copy):
            c(k).wait_send()
        across(lambda d: z_out(k, d).wait_send())
        across(lambda d: r3_copy(k, d).wait_send())

    each(pieces, drain)


def shards(
    gate_in, mult_in, value_in, doc_ids, conv_taps, out_proj, resid, norm1_gain, norm1_bias,
    expert_ids, expert_wts, w_gate, w_up, w_down, norm2_gain, norm2_bias,
):
    experts, parts = lax.axis_size("sp"), lax.axis_size("tp")
    assert parts == 4
    length, channels = mult_in.shape
    count, model = resid.shape
    top = expert_ids.shape[1]
    units = w_gate.shape[2]
    capacity = 5 * count * top // (4 * experts)
    piece = 16
    pieces = -(-capacity // piece)
    slots = pieces * piece
    padded = max(8, experts)
    docs = jnp.broadcast_to(doc_ids[:, None], (length, 128))
    vmem = pl.BlockSpec(memory_space=pltpu.VMEM)
    hbm = pl.BlockSpec(memory_space=pl.ANY)
    V = pltpu.VMEM
    sems = pltpu.SemaphoreType.DMA
    blocks = (pieces, experts, piece, model)
    routed = (pieces, 4, experts, piece, model)
    batch = 4 * experts * piece if 4 * experts * piece <= 512 else experts * piece
    many, each_way = sems((pieces,)), sems((pieces, experts))
    return pl.pallas_call(
        functools.partial(kernel, experts, slots, piece),
        out_shape=jax.ShapeDtypeStruct((count, model), bf16),
        in_specs=[hbm, hbm, hbm, hbm, vmem, hbm, hbm, vmem, vmem, vmem, vmem, hbm, hbm, hbm, vmem, vmem],
        out_specs=vmem,
        scratch_shapes=[
            V((length, channels), bf16), V((length, channels), bf16), V((length, channels), bf16),
            V((length, 128), jnp.int32), V((channels, model), bf16), V((count, model), bf16),
            V((model, units), bf16), V((model, units), bf16), V((units, model), bf16),
            V((16, channels), bf16), V((16, channels), bf16), V((8, 128), jnp.int32),
            V((length + 8, channels), f32), V((length + 8, 128), jnp.int32), V((length, channels), bf16),
            V((2, count, model), bf16), V((2, count, model), bf16), V((count, model), bf16),
            V((count, model), bf16), V((count, model), f32), V((count, model), bf16),
            V((padded, count), f32), V((padded, count), f32),
            V(blocks, bf16), V(routed, bf16), V(routed, bf16), V((batch, units), bf16),
            V((pieces, 2, experts, piece, model), bf16), V(blocks, bf16), V(blocks, bf16), V(blocks, bf16),
            V(blocks, bf16), V((2, pieces, experts, piece, count), bf16),
            sems((9,)), sems((3,)), sems((3,)), sems((3,)), sems((3,)),
            each_way, each_way, many, many, many, many, many, many,
            many, many, many, many, each_way, each_way,
        ],
        compiler_params=pltpu.CompilerParams(
            collective_id=0, has_side_effects=True, vmem_limit_bytes=62 * 2**20
        ),
    )(
        gate_in, mult_in, value_in, docs, conv_taps.astype(f32), out_proj, resid,
        norm1_gain[None], norm1_bias[None], expert_ids.T, expert_wts.T,
        w_gate[0], w_up[0], w_down[0], norm2_gain[None], norm2_bias[None],
    )


def solution(mesh):
    placed = (
        P(("grp", "sp"), "tp"),
        P(("grp", "sp"), "tp"),
        P(("grp", "sp"), "tp"),
        P(("grp", "sp")),
        P(None, "tp"),
        P("tp", None),
        P(("grp", "sp", "tp"), None),
        P(),
        P(),
        P(("grp", "sp", "tp"), None),
        P(("grp", "sp", "tp"), None),
        P("sp", None, "tp"),
        P("sp", None, "tp"),
        P("sp", "tp", None),
        P(),
        P(),
    )
    return jax.shard_map(
        shards, mesh=mesh, in_specs=placed, out_specs=P(("grp", "sp", "tp"), None), check_vma=False
    )
```
